128 devices in a mesh: sp: 64 (over z, y, x), tp: 2 (over core).
Axes of the slice: x: 4, y: 4, z: 4, core: 2. Of those that a mesh axis runs over, the one named last changes fastest.
Arguments:
- queries: bfloat16 [8192, 1024], P('sp', 'tp'), may hold values from -6 to 6
- keys: bfloat16 [8192, 1024], P('sp', 'tp'), may hold values from -6 to 6
- values: bfloat16 [8192, 2048], P('sp', 'tp'), may hold values from -6 to 6
- out_gate: bfloat16 [8192, 2048], P('sp', 'tp'), may hold values from -6 to 6
- decay_rate: float32 [8], P('tp'), may hold values from 0 to 1
- residual: bfloat16 [8192, 2048], P(('sp', 'tp')), may hold values from -6 to 6
- out_weight: bfloat16 [2048, 2048], P('tp'), may hold values from -0.125 to 0.125
- ffn_gain: float32 [2048], replicated, may hold values from 0.1 to 1.9
- route_ids: int32 [8192, 4], P(('sp', 'tp')), may hold values from 0 to 63, all different within a row; in each aligned block of 64 rows (0 to 63, 64 to 127, ...) at most 8 rows name the same one
- route_weights: float32 [8192, 4], P(('sp', 'tp')), may hold values from 0.1 to 1
- gate_up: bfloat16 [64, 2048, 2048], P('sp', None, 'tp'), may hold values from -0.375 to 0.375
- lin_up: bfloat16 [64, 2048, 2048], P('sp', None, 'tp'), may hold values from -0.375 to 0.375
- down_weight: bfloat16 [64, 2048, 2048], P('sp', 'tp'), may hold values from -0.03125 to 0.03125
Outputs:
- layer_out: bfloat16 [8192, 2048], P(('sp', 'tp'))
The draws below stay inside these ranges and needn't reach their ends.
Inputs may be any that keep to these rules, and one draw needn't show every extreme that they name: `route_ids`: within the rows of one device (aligned blocks of 64 rows), no expert is named by more than 8 entries, a bound that some block reaches; the 4 experts of a row differ.
All inputs are finite; a program needn't handle non-finite values.
Results may differ from the reference program's by a relative error of at most 0.03.
Values may be sent and summed in bfloat16 or wider, within the bound.
A program may use at most 128 MiB of HBM per device.

```python
import math
import jax
import jax.numpy as jnp
import numpy as np
from jax import lax

D = 2048
HEADS = 8
DK = 128
DV = 256
DE = 2048
TOPK = 4
TOK_DEV = 128
EXPERTS = 64
TOKENS = 8192
ROWS = 64
CAP = 8
N_SP = 64
N_TP = 2


def draw_decay_rate(key, part):
    first_key, second_key = jax.random.split(key, 2)
    spread = jax.random.uniform(first_key, (HEADS,), jnp.float32)
    slow_low = jnp.log(0.2 / TOKENS)
    slow_high = jnp.log(2.0 / TOKENS)
    fast_low = jnp.log(1.0 / 100.0)
    fast_high = jnp.log(1.0 / 30.0)
    slow_rate = jnp.exp(slow_low + spread * (slow_high - slow_low))
    fast_rate = jnp.exp(fast_low + spread * (fast_high - fast_low))
    order = jax.random.permutation(second_key, HEADS)
    fast_count = HEADS // 2
    return jnp.where(order < fast_count, fast_rate, slow_rate).astype(jnp.float32)


def levels(stream_key, shape, shards, least, largest):
    factor_of, own = 1.0, jax.random.fold_in(stream_key, 6)
    for dim, shards_of in shards:
        steps = jnp.exp(jax.random.uniform(jax.random.fold_in(own, dim), (shards_of,), jnp.float32, least / len(shards), largest / len(shards)))
        factor_of = factor_of * jnp.repeat(steps, shape[dim] // shards_of).reshape([-1 if axis == dim else 1 for axis in range(len(shape))])
    return factor_of


def deal_out(key, own, number, rows, number_of, top, bound, lean):
    sequence = jax.random.permutation(key, number_of)
    heavy_load, usual = load_shares(number_of, rows * top, bound, lean, True), load_shares(number_of, rows * top, bound, lean, False)
    places = jnp.arange(number_of)

    def named(sizes, turn):
        used = int((sizes > 0).sum())
        fixed = max(1, used // 4)
        shifted = fixed + (places - fixed + turn * (used - fixed)) % max(1, number_of - fixed)
        return jnp.zeros((number_of,), jnp.int32).at[sequence[jnp.where(places < fixed, places, shifted)]].set(jnp.asarray(sizes, jnp.int32))

    sizes = jnp.where(number % 4 == 0, named(heavy_load, number // 4), named(usual, number - number // 4 - 1))
    mixed = jax.random.permutation(jax.random.fold_in(own, 3), number_of)
    source_of, sink = mixed[0:number_of // 2 * 2:2], mixed[1:number_of // 2 * 2:2]
    room = jnp.minimum(sizes[source_of] - 1, bound - sizes[sink]) // 2
    room = jnp.where((source_of == sequence[0]) | (sink == sequence[0]) | (sizes[sink] == 0), 0, jnp.maximum(room, 0))
    shifted = jax.random.randint(jax.random.fold_in(own, 4), (number_of // 2,), 0, 1 << 20) % (room + 1)
    sizes = sizes.at[source_of].add(-shifted).at[sink].add(shifted)
    items = jnp.searchsorted(jnp.cumsum(sizes), jnp.arange(rows * top), side="right").astype(jnp.int32)
    table = items.reshape(top, rows).T
    table = table[jax.random.permutation(jax.random.fold_in(own, 1), rows)]
    turn = jax.random.randint(jax.random.fold_in(own, 2), (rows, 1), 0, top)
    return jnp.take_along_axis(table, (jnp.arange(top)[None, :] + turn) % top, axis=1)


def load_shares(amount, total, limit, slope, full):
    loads = [(1 << 20) // math.isqrt(standing ** slope) + 1 for standing in range(1, amount + 1)]
    largest = limit if full else min(limit, max(-(-total // amount), total * loads[0] // sum(loads)))
    least = 1 if total - largest >= amount - 1 else 0
    given, surplus = [largest] + [least] * (amount - 1), total - largest - least * (amount - 1)
    while surplus > 0:
        free = [i for i in range(1, amount) if given[i] < largest] or [i for i in range(1, amount) if given[i] < limit]
        pool, left = sum([loads[i] for i in free]), surplus
        for i in free:
            extra = min(limit - given[i], max(1, left * loads[i] // pool), surplus)
            given[i] = given[i] + extra
            surplus = surplus - extra
    return np.array(given)


def gaussian(own_key, extent, scale, most, cuts=(), kind=jnp.bfloat16):
    drawn = jax.random.normal(own_key, extent, jnp.float32) * scale
    if len(cuts) > 0:
        drawn = levels(own_key, extent, cuts, -0.22, 0.18) * drawn
    return jnp.clip(drawn, min=-most, max=most).astype(kind)


def setup_inputs(seed: int = 0) -> dict:
    streams_of = jax.random.split(jax.random.key(seed), 14)
    queries = gaussian(streams_of[0], (TOKENS, HEADS * DK), 1.0, 6.0, ((0, 64), (1, 2)))
    keys = gaussian(streams_of[1], (TOKENS, HEADS * DK), 1.0, 6.0, ((0, 64), (1, 2)))
    values = gaussian(streams_of[2], (TOKENS, HEADS * DV), 1.0, 6.0, ((0, 64), (1, 2)))
    out_gate = gaussian(streams_of[3], (TOKENS, HEADS * DV), 1.0, 6.0, ((0, 64), (1, 2)))
    decay_rate = draw_decay_rate(jax.random.fold_in(streams_of[13], 71), 0)
    residual = gaussian(streams_of[5], (TOKENS, D), 1.0, 6.0, ((0, 128),))
    out_weight = gaussian(streams_of[6], (HEADS * DV, D), (HEADS * DV) ** -0.5, 0.125, ((0, 2),))
    ffn_gain = jnp.clip(1.0 + 0.18 * jax.random.normal(streams_of[7], (D,), jnp.float32), 0.1, 1.9)
    route_ids_keys = jax.random.split(jax.random.fold_in(streams_of[8], 1), TOKENS // ROWS)
    route_ids_turns = jax.random.permutation(jax.random.fold_in(streams_of[8], 3), TOKENS // ROWS)
    route_ids = jax.vmap(lambda own, number: deal_out(jax.random.fold_in(streams_of[8], 2), own, number, ROWS, EXPERTS, TOPK, CAP, 1))(route_ids_keys, route_ids_turns).reshape((TOKENS, TOPK))
    route_weights = jnp.clip(jnp.exp(math.log(1.0) - 2.3025851 * jax.random.uniform(streams_of[9], (TOKENS, TOPK), jnp.float32) ** levels(streams_of[9], (TOKENS, TOPK), ((0, 128),), -0.2, 0.2)), 0.1, 1.0)
    gate_up = gaussian(streams_of[10], (EXPERTS, D, DE), (D // 9) ** -0.5, 0.375, ((0, 64), (2, 2)))
    lin_up = gaussian(streams_of[11], (EXPERTS, D, DE), (D // 9) ** -0.5, 0.375, ((0, 64), (2, 2)))
    down_weight = gaussian(streams_of[12], (EXPERTS, DE, D), (DE * 16) ** -0.5, 0.03125, ((0, 64), (1, 2)))
    return dict(queries=queries, keys=keys, values=values, out_gate=out_gate, decay_rate=decay_rate, residual=residual, out_weight=out_weight, ffn_gain=ffn_gain, route_ids=route_ids, route_weights=route_weights, gate_up=gate_up, lin_up=lin_up, down_weight=down_weight)


EPS = 1e-05
CLAMP_LIMIT = 7.0
SIGMOID_SLOPE = 1.702
TOP_PRECISION = lax.Precision.HIGHEST

def expert_act(row_block, gate_part, lin_part):
    gate_pre = jnp.dot(row_block, gate_part, preferred_element_type=jnp.float32)
    lin_pre = jnp.dot(row_block, lin_part, preferred_element_type=jnp.float32)
    gate_clip = jnp.minimum(gate_pre, CLAMP_LIMIT)
    lin_clip = jnp.clip(lin_pre, -CLAMP_LIMIT, CLAMP_LIMIT)
    return (gate_clip * jax.nn.sigmoid(SIGMOID_SLOPE * gate_clip) * (lin_clip + 1.0)).astype(jnp.bfloat16)

def reference(queries, keys, values, out_gate, decay_rate, residual, out_weight, ffn_gain, route_ids, route_weights, gate_up, lin_up, down_weight):
    total_tokens = queries.shape[0]
    block_len = TOK_DEV
    block_count = total_tokens // block_len
    log_gamma = -decay_rate.astype(jnp.float32)
    query_heads = queries.astype(jnp.float32).reshape(block_count, block_len, HEADS, DK).transpose(0, 2, 1, 3)
    per_head_keys = keys.astype(jnp.float32).reshape(block_count, block_len, HEADS, DK).transpose(0, 2, 1, 3) * DK ** (-0.5)
    per_head_values = values.astype(jnp.float32).reshape(block_count, block_len, HEADS, DV).transpose(0, 2, 1, 3)
    positions = jnp.arange(block_len, dtype=jnp.float32)
    offsets = positions[:, None] - positions[None, :]
    causal = offsets >= 0
    decay_mask = jnp.where(causal[None], jnp.exp(jnp.where(causal, offsets, 0.0)[None] * log_gamma[:, None, None]), 0.0)
    trailing_decay = jnp.exp((block_len - 1.0 - positions)[None, :] * log_gamma[:, None])
    lead_decay = jnp.exp((positions + 1.0)[None, :] * log_gamma[:, None])
    chain_decay = jnp.exp(block_len * log_gamma)

    def block_step(carried, block):
        query_block, block_keys, block_values = block
        attention_scores = jnp.einsum('hqd,hkd->hqk', query_block, block_keys, precision=TOP_PRECISION) * decay_mask
        intra_block_term = jnp.einsum('zfp,zpn->zfn', attention_scores, block_values, precision=TOP_PRECISION)
        cross_term = jnp.einsum('hqd,hdv->hqv', query_block, carried, precision=TOP_PRECISION) * lead_decay[:, :, None]
        state_delta = jnp.einsum('mxs,mxq->msq', block_keys * trailing_decay[:, :, None], block_values, precision=TOP_PRECISION)
        new_state = chain_decay[:, None, None] * carried + state_delta
        return (new_state, intra_block_term + cross_term)
    _, outputs = lax.scan(block_step, jnp.zeros((HEADS, DK, DV), jnp.float32), (query_heads, per_head_keys, per_head_values))
    retained = outputs.transpose(0, 2, 1, 3).reshape(total_tokens, HEADS, DV)
    normed = retained * lax.rsqrt(lax.optimization_barrier(jnp.mean(retained * retained, axis=-1, keepdims=True)) + EPS)
    gated = (normed.reshape(total_tokens, HEADS * DV) * jax.nn.silu(out_gate.astype(jnp.float32))).astype(jnp.bfloat16)
    group_width = HEADS * DV // N_TP
    mix_rows = jnp.zeros((total_tokens, D), jnp.float32)
    for group in range(N_TP):
        partial_value = jnp.dot(gated[:, group * group_width:(group + 1) * group_width], out_weight[group * group_width:(group + 1) * group_width], preferred_element_type=jnp.float32).astype(jnp.bfloat16)
        mix_rows = mix_rows + lax.optimization_barrier(partial_value).astype(jnp.float32)
    mixed = (residual.astype(jnp.float32) + mix_rows).astype(jnp.bfloat16)
    mixed_wide = mixed.astype(jnp.float32)
    normed_rows = (mixed_wide * lax.rsqrt(lax.optimization_barrier(jnp.mean(mixed_wide * mixed_wide, axis=-1, keepdims=True)) + EPS) * ffn_gain.astype(jnp.float32)).astype(jnp.bfloat16)
    device_count = N_SP * N_TP
    own_rows = total_tokens // device_count
    block_ids = route_ids.reshape(device_count, own_rows * TOPK).astype(jnp.int32)
    one_hot = (block_ids[:, :, None] == jnp.arange(EXPERTS, dtype=jnp.int32)[None, None, :]).astype(jnp.int32)
    slot_rank = lax.optimization_barrier(jnp.sum(one_hot * (jnp.cumsum(one_hot, axis=1) - 1), axis=2))
    device_index = jnp.arange(device_count, dtype=jnp.int32)[:, None]
    slot_index = (block_ids * (device_count * CAP) + device_index * CAP + slot_rank).reshape(-1).astype(jnp.int32)
    source_row = (jnp.arange(total_tokens * TOPK, dtype=jnp.int32) // TOPK).astype(jnp.int32)
    slot_source = jnp.full((EXPERTS * device_count * CAP,), total_tokens, jnp.int32).at[slot_index].set(source_row)
    padded = jnp.concatenate([normed_rows, jnp.zeros((1, D), jnp.bfloat16)], axis=0)
    half_width = DE // N_TP

    def run_expert(packed):
        sources, gate_full, lin_full, down_full = packed
        activation = expert_act(padded[sources], gate_full, lin_full)
        summed = jnp.zeros((sources.shape[0], D), jnp.float32)
        for group in range(N_TP):
            partial_value = jnp.dot(activation[:, group * half_width:(group + 1) * half_width], down_full[group * half_width:(group + 1) * half_width], preferred_element_type=jnp.float32).astype(jnp.bfloat16)
            summed = summed + lax.optimization_barrier(partial_value).astype(jnp.float32)
        return summed.astype(jnp.bfloat16)
    results = lax.map(run_expert, (slot_source.reshape(EXPERTS, device_count * CAP), gate_up, lin_up, down_weight))
    picked = results.reshape(-1, D)[slot_index].reshape(total_tokens, TOPK, D).astype(jnp.float32)
    expert_sum = lax.optimization_barrier(jnp.sum(picked * route_weights.astype(jnp.float32)[:, :, None], axis=1))
    return (mixed.astype(jnp.float32) + expert_sum).astype(jnp.bfloat16)
```

```python
import jax
import jax.numpy as jnp
from jax import lax
from jax.sharding import Mesh
from jax.sharding import PartitionSpec as P

D = 2048
DK = 128
DV = 256
SP = ("sp_0", "sp_1", "sp_2")
SP_TP = ("sp_0", "sp_1", "sp_2", "tp")


EPS = 1e-05
CLAMP_LIMIT = 7.0
SIGMOID_SLOPE = 1.702
TOP_PRECISION = lax.Precision.HIGHEST


def carried_state(state_delta, log_gamma, block_len):
    peers, mine = (lax.axis_size(SP), lax.axis_index(SP))
    heads = state_delta.shape[0]
    pieces = state_delta.astype(jnp.bfloat16).reshape(peers, -1)
    arrived = lax.all_to_all(pieces, SP, split_axis=0, concat_axis=0, tiled=True)
    own_log = lax.dynamic_index_in_dim(log_gamma, mine * heads // peers, keepdims=False)
    order = jnp.arange(peers, dtype=jnp.float32)
    gap = order[:, None] - 1.0 - order[None, :]
    weight = jnp.where(gap >= 0, jnp.exp(jnp.maximum(gap, 0.0) * block_len * own_log), 0.0)
    before = jnp.dot(weight, arrived.astype(jnp.float32), precision=TOP_PRECISION)
    returned = lax.all_to_all(
        before.astype(jnp.bfloat16), SP, split_axis=0, concat_axis=0, tiled=True
    )
    return returned.reshape(state_delta.shape).astype(jnp.float32)


def in_blocks(array, dim, peers):
    before, after = (array.shape[:dim], array.shape[dim + 1 :])
    return jnp.moveaxis(array.reshape(*before, peers, -1, *after), dim, 0)


def summed_on_arrival(array, axis, dim):
    tiles = in_blocks(array, dim, lax.axis_size(axis))
    arrived = lax.all_to_all(tiles, axis, split_axis=0, concat_axis=0, tiled=True)
    return arrived.astype(jnp.float32).sum(axis=0)


def expert_act(row_block, gate_part, lin_part):
    gate_pre = jnp.dot(row_block, gate_part, preferred_element_type=jnp.float32)
    lin_pre = jnp.dot(row_block, lin_part, preferred_element_type=jnp.float32)
    gate_clip = jnp.minimum(gate_pre, CLAMP_LIMIT)
    lin_clip = jnp.clip(lin_pre, -CLAMP_LIMIT, CLAMP_LIMIT)
    return (gate_clip * jax.nn.sigmoid(SIGMOID_SLOPE * gate_clip) * (lin_clip + 1.0)).astype(
        jnp.bfloat16
    )


def local(
    queries,
    keys,
    values,
    out_gate,
    decay_rate,
    residual,
    out_weight,
    ffn_gain,
    route_ids,
    route_weights,
    gate_up,
    lin_up,
    down_weight,
):
    block_len = queries.shape[0]
    local_heads = decay_rate.shape[0]
    log_gamma = -decay_rate
    query_heads = queries.astype(jnp.float32).reshape(block_len, local_heads, DK).transpose(1, 0, 2)
    per_head_keys = keys.astype(jnp.float32).reshape(block_len, local_heads, DK).transpose(
        1, 0, 2
    ) * DK ** (-0.5)
    per_head_values = (
        values.astype(jnp.float32).reshape(block_len, local_heads, DV).transpose(1, 0, 2)
    )
    positions = jnp.arange(block_len, dtype=jnp.float32)
    offsets = positions[:, None] - positions[None, :]
    causal = offsets >= 0
    decay_mask = jnp.where(
        causal[None], jnp.exp(jnp.where(causal, offsets, 0.0)[None] * log_gamma[:, None, None]), 0.0
    )
    trailing_decay = jnp.exp((block_len - 1.0 - positions)[None, :] * log_gamma[:, None])
    lead_decay = jnp.exp((positions + 1.0)[None, :] * log_gamma[:, None])
    attention_scores = (
        jnp.einsum("hqd,hkd->hqk", query_heads, per_head_keys, precision=TOP_PRECISION) * decay_mask
    )
    intra_block_term = jnp.einsum(
        "zfp,zpn->zfn", attention_scores, per_head_values, precision=TOP_PRECISION
    )
    state_delta = jnp.einsum(
        "mxs,mxq->msq",
        per_head_keys * trailing_decay[:, :, None],
        per_head_values,
        precision=TOP_PRECISION,
    )
    carried = carried_state(state_delta, log_gamma, block_len)
    cross_term = (
        jnp.einsum("hqd,hdv->hqv", query_heads, carried, precision=TOP_PRECISION)
        * lead_decay[:, :, None]
    )
    retained = intra_block_term + cross_term
    normed = retained * lax.rsqrt(jnp.mean(retained * retained, axis=-1, keepdims=True) + EPS)
    gated = (
        normed.transpose(1, 0, 2).reshape(block_len, local_heads * DV)
        * jax.nn.silu(out_gate.astype(jnp.float32))
    ).astype(jnp.bfloat16)
    mix_rows = summed_on_arrival(
        jnp.dot(gated, out_weight, preferred_element_type=jnp.float32).astype(jnp.bfloat16), "tp", 0
    )
    mixed = (residual.astype(jnp.float32) + mix_rows).astype(jnp.bfloat16)
    mixed_wide = mixed.astype(jnp.float32)
    normed_rows = (
        mixed_wide
        * lax.rsqrt(jnp.mean(mixed_wide * mixed_wide, axis=-1, keepdims=True) + EPS)
        * ffn_gain
    ).astype(jnp.bfloat16)
    experts = lax.axis_size(SP)
    own_rows = route_ids.shape[0]
    top_count = route_ids.shape[1]
    capacity = own_rows * top_count * lax.axis_size("tp") // experts
    flat_ids = route_ids.reshape(-1)
    one_hot = (flat_ids[:, None] == jnp.arange(experts, dtype=jnp.int32)[None, :]).astype(jnp.int32)
    slot_rank = jnp.sum(one_hot * (jnp.cumsum(one_hot, axis=0) - 1), axis=1)
    slot_index = flat_ids * capacity + slot_rank
    source_row = jnp.arange(own_rows * top_count, dtype=jnp.int32) // top_count
    slot_source = (
        jnp.full((experts * capacity,), own_rows, jnp.int32).at[slot_index].set(source_row)
    )
    padded = jnp.concatenate([normed_rows, jnp.zeros((1, D), jnp.bfloat16)], axis=0)
    outgoing = padded[slot_source].reshape(experts, capacity, D)
    gate_half = gate_up[0]
    lin_half = lin_up[0]
    down_half = down_weight[0]
    pair_rows = lax.all_gather(
        lax.all_to_all(outgoing, SP, split_axis=0, concat_axis=0, tiled=True),
        "tp",
        axis=0,
        tiled=True,
    )
    activation = expert_act(pair_rows.reshape(-1, D), gate_half, lin_half)
    partial_value = jnp.dot(activation, down_half, preferred_element_type=jnp.float32).reshape(
        pair_rows.shape
    )
    summed = summed_on_arrival(partial_value.astype(jnp.bfloat16), "tp", 0)
    returned = lax.all_to_all(
        summed.astype(jnp.bfloat16), SP, split_axis=0, concat_axis=0, tiled=True
    )
    picked = (
        returned.reshape(experts * capacity, D)[slot_index]
        .reshape(own_rows, top_count, D)
        .astype(jnp.float32)
    )
    expert_sum = jnp.sum(picked * route_weights[:, :, None], axis=1)
    return (mixed_wide + expert_sum).astype(jnp.bfloat16)


def solution(mesh):
    torus = Mesh(mesh.devices.reshape(4, 4, 4, mesh.shape["tp"]), ("sp_0", "sp_1", "sp_2", "tp"))
    in_specs = (
        P(SP, "tp"),
        P(SP, "tp"),
        P(SP, "tp"),
        P(SP, "tp"),
        P("tp"),
        P(SP_TP, None),
        P("tp", None),
        P(),
        P(SP_TP, None),
        P(SP_TP, None),
        P(SP, None, "tp"),
        P(SP, None, "tp"),
        P(SP, "tp", None),
    )
    out_specs = P(SP_TP, None)
    return jax.shard_map(local, mesh=torus, in_specs=in_specs, out_specs=out_specs, check_vma=False)
```
